256 devices in a mesh: sp: 32 (over z, y), tp: 8 (over x, core).
Axes of the slice: x: 4, y: 4, z: 8, core: 2. Of those that a mesh axis runs over, the one named last changes fastest.
Arguments:
- tokens: bfloat16 [32768, 4096], P('sp', 'tp'), may hold values from -6 to 6
- norm_gain: float32 [4096], replicated, may hold values from 0.1 to 1.9
- pool_in_weight: bfloat16 [4096, 2048], P('sp', 'tp'), may hold values from -0.09375 to 0.09375
- query_weight: bfloat16 [4096, 2048], P('sp', 'tp'), may hold values from -1 to 1, as said below
- key_weight: bfloat16 [4096, 512], P('sp', 'tp'), may hold values from -40 to 40
- value_weight: bfloat16 [4096, 512], P('sp', 'tp'), may hold values from -0.09375 to 0.09375
- pool_weight: bfloat16 [8, 256, 256], P('tp'), may hold values from -0.375 to 0.375
- pool_scale: float32 [2048], P('tp'), may hold values from 0.1 to 1.9
- sink_logit: float32 [32], P('tp'), may hold values from 3 to 7
- out_pool_weight: bfloat16 [2048, 4096], P('tp', 'sp'), may hold values from -0.09375 to 0.09375
- out_attn_weight: bfloat16 [2048, 4096], P('tp', 'sp'), may hold values from -1.5 to 1.5
Outputs:
- mixed: bfloat16 [32768, 4096], P(('sp', 'tp'))
The draws below stay inside these ranges and needn't reach their ends.
Inputs may be any that keep to these rules, and one draw needn't show every extreme that they name: `query_weight`: entries of order 4096 ** -0.5, drawn independently.
All inputs are finite; a program needn't handle non-finite values.
Results may differ from the reference program's by a relative error of at most 0.014.
The reference program's roundings to bfloat16 on the way count: a program that leaves them out, or rounds other values in their place, can miss the bound.
Values may be sent and summed in bfloat16 or wider, within the bound.
No kernel may reach another device: no remote copies, remote signals or barrier semaphores. Data moves between devices by JAX's collectives and lax.ppermute only.
A program may use at most 128 MiB of HBM per device.

```python
import jax
import jax.numpy as jnp
from jax import lax

D = 4096
HEAD_DIM = 64
Q_HEADS = 32
KV_HEADS = 8
POOL_GROUPS = 8
GROUP_DIM = 256
WINDOW = 128
GRID_W = 64
TOK_DEV = 1024
TOKENS = 32768
POOL_WIDTH = 2048
ATTN_WIDTH = 2048
KV_WIDTH = 512
N_TP = 8


def weight_pair(key):
    query_part = jax.random.normal(jax.random.fold_in(key, 11), (D, ATTN_WIDTH), jnp.float32) * D ** (-0.5)
    key_part = jax.random.normal(jax.random.fold_in(key, 12), (D, KV_WIDTH), jnp.float32) * D ** (-0.5)
    return (query_part, key_part)


def draw_query_weight(key, part):
    return weight_pair(key)[0].astype(jnp.bfloat16)


def draw_key_weight(key, part):
    query_part, key_part = weight_pair(key)
    return key_part.astype(jnp.bfloat16)


def shard_levels(key, extent, pieces, smallest, high):
    level, own = 1.0, jax.random.fold_in(key, 6)
    for position, shards_of in pieces:
        heights = jnp.exp(jax.random.uniform(jax.random.fold_in(own, position), (shards_of,), jnp.float32, smallest / len(pieces), high / len(pieces)))
        level = level * jnp.repeat(heights, extent[position] // shards_of).reshape([-1 if axis == position else 1 for axis in range(len(extent))])
    return level


def noise(key, dims, width, reach, cuts=(), held_as=jnp.bfloat16):
    values = jax.random.normal(key, dims, jnp.float32) * width
    if len(cuts) > 0:
        values = shard_levels(key, dims, cuts, -0.22, 0.18) * values
    return jnp.clip(values, min=-reach, max=reach).astype(held_as)


def setup_inputs(seed: int = 0) -> dict:
    seeds = jax.random.split(jax.random.key(seed), 12)
    tokens = noise(seeds[0], (TOKENS, D), 1.0, 6.0, ((0, 32), (1, 8)))
    norm_gain = jnp.clip(1.0 + 0.18 * jax.random.normal(seeds[1], (D,), jnp.float32), 0.1, 1.9)
    pool_in_weight = noise(seeds[2], (D, POOL_WIDTH), D ** -0.5, 0.09375, ((0, 32), (1, 8)))
    query_weight = draw_query_weight(jax.random.fold_in(seeds[11], 71), 0)
    key_weight = draw_key_weight(jax.random.fold_in(seeds[11], 71), 0)
    value_weight = noise(seeds[5], (D, KV_WIDTH), D ** -0.5, 0.09375, ((0, 32), (1, 8)))
    pool_weight = noise(seeds[6], (POOL_GROUPS, GROUP_DIM, GROUP_DIM), GROUP_DIM ** -0.5, 0.375, ((0, 8),))
    pool_scale = jnp.clip(1.0 + 0.18 * jax.random.normal(seeds[7], (POOL_WIDTH,), jnp.float32), 0.1, 1.9)
    sink_logit = jnp.clip(3.0 + 4.0 * jax.random.uniform(seeds[8], (Q_HEADS,), jnp.float32) ** shard_levels(seeds[8], (Q_HEADS,), ((0, 8),), -0.2, 0.2), 3.0, 7.0)
    out_pool_weight = noise(seeds[9], (POOL_WIDTH, D), (2 * POOL_WIDTH) ** -0.5, 0.09375, ((0, 8), (1, 32)))
    out_attn_weight = noise(seeds[10], (ATTN_WIDTH, D), (ATTN_WIDTH // 128) ** -0.5, 1.5, ((0, 8), (1, 32)))
    return dict(tokens=tokens, norm_gain=norm_gain, pool_in_weight=pool_in_weight, query_weight=query_weight, key_weight=key_weight, value_weight=value_weight, pool_weight=pool_weight, pool_scale=pool_scale, sink_logit=sink_logit, out_pool_weight=out_pool_weight, out_attn_weight=out_attn_weight)


epsilon = 1e-06
rotary_base = 10000.0
masked_score = -1e+30

def rms_normed(values, gain):
    floats = values.astype(jnp.float32)
    scaled = floats * lax.rsqrt(lax.optimization_barrier(jnp.mean(floats * floats, axis=-1, keepdims=True)) + epsilon)
    return (scaled * gain).astype(jnp.bfloat16)

def rotary_tables(positions, head_dim, grid_width):
    freq_count = head_dim // 4
    inverse = rotary_base ** (-jnp.arange(freq_count, dtype=jnp.float32) / freq_count)
    row_pos = (positions // grid_width).astype(jnp.float32)
    col_pos = (positions % grid_width).astype(jnp.float32)
    angles = jnp.stack([row_pos[:, None] * inverse, col_pos[:, None] * inverse], axis=1)
    return (jnp.cos(angles), jnp.sin(angles))

def rotate(values, cosine, sine):
    length, heads, head_dim = values.shape
    split = values.reshape(length, heads, 2, 2, head_dim // 4)
    first = split[:, :, :, 0]
    second = split[:, :, :, 1]
    cos_b = cosine[:, None]
    sin_b = sine[:, None]
    turned = jnp.stack([first * cos_b - second * sin_b, second * cos_b + first * sin_b], axis=3)
    return turned.reshape(length, heads, head_dim)

def pool_branch(pool_in, pool_weight, pool_scale):
    length, channels = pool_in.shape
    running = jnp.concatenate([jnp.zeros((1, channels), jnp.float32), jnp.cumsum(pool_in.astype(jnp.float32), axis=0)], axis=0)
    group_ids = jnp.arange(channels, dtype=jnp.int32) // GROUP_DIM
    halves = jnp.array([1, 2, 4, 8], jnp.int32)[group_ids % 4]
    positions = jnp.arange(length, dtype=jnp.int32)[:, None]
    lower = jnp.clip(positions - halves[None, :], 0, length).astype(jnp.int32)
    upper = jnp.clip(positions + halves[None, :], 0, length).astype(jnp.int32)
    window_sum = jnp.take_along_axis(running, upper, 0) - jnp.take_along_axis(running, lower, 0)
    window_mean = window_sum / (upper - lower).astype(jnp.float32)
    pooled = (window_mean - pool_in.astype(jnp.float32)).astype(jnp.bfloat16)
    grouped = pooled.reshape(length, channels // GROUP_DIM, GROUP_DIM).astype(jnp.float32)
    mixing = jnp.einsum('lgc,gcd->lgd', grouped, pool_weight.astype(jnp.float32))
    return (mixing.reshape(length, channels) * pool_scale).astype(jnp.bfloat16)

def attention_branch(queries, key_rows, value_rows, sink_logit, block):
    length = queries.shape[0]
    group = Q_HEADS // KV_HEADS
    pad_keys = jnp.pad(key_rows, ((WINDOW, WINDOW), (0, 0), (0, 0)))
    pad_values = jnp.pad(value_rows, ((WINDOW, WINDOW), (0, 0), (0, 0)))
    span = block + 2 * WINDOW

    def one_block(index):
        start = (index * block).astype(jnp.int32)
        query_block = lax.dynamic_slice_in_dim(queries, start, block, 0).astype(jnp.float32)
        query_block = query_block.reshape(block, KV_HEADS, group, HEAD_DIM)
        key_block = lax.dynamic_slice_in_dim(pad_keys, start, span, 0).astype(jnp.float32)
        value_block = lax.dynamic_slice_in_dim(pad_values, start, span, 0).astype(jnp.float32)
        scores = jnp.einsum('qkgd,skd->kgqs', query_block, key_block) * HEAD_DIM ** (-0.5)
        query_pos = start + jnp.arange(block, dtype=jnp.int32)
        key_pos = start - WINDOW + jnp.arange(span, dtype=jnp.int32)
        allowed = (jnp.abs(key_pos[None, :] - query_pos[:, None]) <= WINDOW) & (key_pos >= 0)[None, :] & (key_pos < length)[None, :]
        scores = jnp.where(allowed, scores, masked_score)
        sink = jnp.broadcast_to(sink_logit.reshape(KV_HEADS, group, 1, 1), scores.shape[:-1] + (1,))
        weights = jax.nn.softmax(jnp.concatenate([scores, sink], axis=-1), axis=-1)[..., :-1]
        weights = weights.astype(jnp.bfloat16).astype(jnp.float32)
        output = jnp.einsum('kgqs,skd->qkgd', weights, value_block)
        return output.reshape(block, Q_HEADS * HEAD_DIM).astype(jnp.bfloat16)
    blocks = lax.map(one_block, jnp.arange(length // block, dtype=jnp.int32))
    return blocks.reshape(length, Q_HEADS * HEAD_DIM)

def reference(tokens, norm_gain, pool_in_weight, query_weight, key_weight, value_weight, pool_weight, pool_scale, sink_logit, out_pool_weight, out_attn_weight):
    length = tokens.shape[0]
    normed = rms_normed(tokens, norm_gain)
    pool_in = jnp.dot(normed, pool_in_weight, preferred_element_type=jnp.float32).astype(jnp.bfloat16)
    positions = jnp.arange(length, dtype=jnp.int32)
    cosine, sine = rotary_tables(positions, HEAD_DIM, GRID_W)
    query_raw = jnp.dot(normed, query_weight, preferred_element_type=jnp.float32)
    queries = rotate(query_raw.reshape(length, Q_HEADS, HEAD_DIM), cosine, sine).astype(jnp.bfloat16)
    key_raw = jnp.dot(normed, key_weight, preferred_element_type=jnp.float32)
    key_rows = rotate(key_raw.reshape(length, KV_HEADS, HEAD_DIM), cosine, sine).astype(jnp.bfloat16)
    value_rows = jnp.dot(normed, value_weight, preferred_element_type=jnp.float32).astype(jnp.bfloat16)
    value_rows = value_rows.reshape(length, KV_HEADS, HEAD_DIM)
    pool_out = pool_branch(pool_in, pool_weight, pool_scale)
    attn_out = attention_branch(queries, key_rows, value_rows, sink_logit, TOK_DEV)
    pool_share = POOL_WIDTH // N_TP
    attn_share = ATTN_WIDTH // N_TP
    mixed = jnp.zeros((length, D), jnp.float32)
    for index in range(N_TP):
        partial_value = jnp.dot(pool_out[:, index * pool_share:(index + 1) * pool_share], out_pool_weight[index * pool_share:(index + 1) * pool_share], preferred_element_type=jnp.float32)
        partial_value = partial_value + jnp.dot(attn_out[:, index * attn_share:(index + 1) * attn_share], out_attn_weight[index * attn_share:(index + 1) * attn_share], preferred_element_type=jnp.float32)
        mixed = mixed + partial_value.astype(jnp.bfloat16).astype(jnp.float32)
    return mixed.astype(jnp.bfloat16)
```

```python
import functools

import jax
import jax.numpy as jnp
from jax import lax
from jax.experimental import pallas as pl
from jax.experimental.pallas import tpu as pltpu
from jax.sharding import Mesh
from jax.sharding import PartitionSpec as P


NZ, NY, NX, NC = 8, 4, 4, 2
HEAD_DIM = 64
GROUP = 4
WINDOW = 128
GRID_W = 64
REACH = 8
ROWS = 1024
TOTAL = ROWS * NZ * NY
BLK = 128
POOL_W = 256
Q_W = 256
KV_W = 128
IN_W = POOL_W + Q_W + KV_W
D = 4096
epsilon = 1e-06
rotary_base = 10000.0
masked_score = -1e30
F32 = jnp.float32
BF16 = jnp.bfloat16


def shift(array, axis, size, step):
    return lax.ppermute(array, axis, [(i, (i + step) % size) for i in range(size)])


def dot(a, b):
    return jnp.dot(a, b, preferred_element_type=F32)


def vmem():
    return pl.BlockSpec(memory_space=pltpu.VMEM)


def smem():
    return pl.BlockSpec(memory_space=pltpu.SMEM)


PARAMS = pltpu.CompilerParams(vmem_limit_bytes=20 * 1024 * 1024)
GRID_PARAMS = pltpu.CompilerParams(
    dimension_semantics=("arbitrary",), vmem_limit_bytes=20 * 1024 * 1024
)


def one_way(array, axis, step):
    size = {"x": NX, "y": NY, "z": NZ}[axis]
    pairs = []
    for i in range(size):
        for c, sign in enumerate((1, -1)):
            pairs.append((i * NC + c, (i + sign * step) % size * NC + c))
    return lax.ppermute(array, (axis, "c"), pairs)


def both_ways(block, axis, size):
    out = {0: block}
    ahead = behind = block
    for k in range(1, size // 2):
        ahead = out[k] = one_way(ahead, axis, 1)
        behind = out[size - k] = one_way(behind, axis, -1)
    out[size // 2] = one_way(ahead, axis, 1)
    return [out[k] for k in range(size)]


def pack_kernel(*refs):
    pieces, out = refs[:-1], refs[-1]
    rows = pieces[0].shape[0]
    for k, piece in enumerate(pieces):
        out[k * rows : (k + 1) * rows, :] = piece[...]


def packed(pieces):
    rows, width = pieces[0].shape
    return pl.pallas_call(
        pack_kernel,
        in_specs=[vmem()] * len(pieces),
        out_specs=vmem(),
        out_shape=jax.ShapeDtypeStruct((rows * len(pieces), width), BF16),
        compiler_params=PARAMS,
        name="pack",
    )(*pieces)


def signed(c, value, size):
    return lax.rem(jnp.where(c == 0, value, -value) + 2 * size, size)


def norm_kernel(place, *refs):
    shards, (gain, out) = refs[:8], refs[8:]
    z, y, x, c = place[0], place[1], place[2], place[3]


    def some(r, carry):
        rows = pl.ds(pl.multiple_of(r * 32, 32), 32)
        values = [shard[rows, :].astype(F32) for shard in shards]
        square = sum(v * v for v in values)
        scale = lax.rsqrt(jnp.sum(square, axis=-1, keepdims=True) * (1.0 / D) + epsilon)
        for k, v in enumerate(values):
            core = c if k % 2 == 0 else 1 - c
            chip = lax.rem(x - jnp.where(core == 0, k // 2, -(k // 2)) + NX, NX)
            zz = chip * NC + core
            g = gain[:, pl.ds(pl.multiple_of(zz * 512, 512), 512)]
            n = ((v * scale) * g).astype(BF16)
            slot = signed(c, z - zz, NZ)
            for yy in range(NY):
                line = signed(c, y - yy, NY)
                out[line, rows, pl.ds(pl.multiple_of(slot * BLK, BLK), BLK)] = n[
                    :, yy * BLK : (yy + 1) * BLK
                ]
        return carry

    lax.fori_loop(0, BLK // 32, some, 0)


def normed_rows(place, shards, gain):
    block = pl.BlockSpec((BLK, 512), lambda i: (i, 0))
    return pl.pallas_call(
        norm_kernel,
        grid=(ROWS // BLK,),
        in_specs=[smem()] + [block] * 8 + [pl.BlockSpec((1, D), lambda i: (0, 0))],
        out_specs=pl.BlockSpec((NY, BLK, NZ * BLK), lambda i: (0, i, 0)),
        out_shape=jax.ShapeDtypeStruct((NY, ROWS, NZ * BLK), BF16),
        compiler_params=GRID_PARAMS,
        name="norm",
    )(place, *shards, gain.reshape(1, D))


def first_kernel(n0, n1, n2, w0, w1, w2, acc):
    acc[...] = dot(n0[0], w0[...]) + dot(n1[0], w1[...]) + dot(n2[0], w2[...])


TILE = 256


def line_spec(line):
    return pl.BlockSpec((1, TILE, NZ * BLK), lambda i: (line, i, 0))


def first_projection(normed, w0, w1, w2):
    whole = pl.BlockSpec((NZ * BLK, IN_W), lambda i: (0, 0))
    return pl.pallas_call(
        first_kernel,
        grid=(ROWS // TILE,),
        in_specs=[line_spec(0), line_spec(1), line_spec(3), whole, whole, whole],
        out_specs=pl.BlockSpec((TILE, IN_W), lambda i: (i, 0)),
        out_shape=jax.ShapeDtypeStruct((ROWS, IN_W), F32),
        compiler_params=GRID_PARAMS,
        name="project_first",
    )(normed, normed, normed, w0, w1, w2)


def turn(v, cosine, sine):
    lane = lax.broadcasted_iota(jnp.int32, v.shape, 1)
    even = (lane // 16) % 2 == 0
    other = jnp.where(even, pltpu.roll(v, 112, 1), pltpu.roll(v, 16, 1))
    return v * cosine + other * sine


def second_kernel(n3, w3, acc, cos, sin, pool, query, kv, low, high):
    step = pl.program_id(0)
    raw = acc[...] + dot(n3[0], w3[...])
    pool_in = raw[:, :POOL_W].astype(BF16)
    pool[...] = pool_in
    c, s = cos[...], sin[...]
    factor = jnp.asarray(HEAD_DIM**-0.5, BF16)
    query[:, :128] = turn(raw[:, 256:384], c, s).astype(BF16) * factor
    query[:, 128:] = turn(raw[:, 384:512], c, s).astype(BF16) * factor
    both = raw[:, 512:640]
    lane = lax.broadcasted_iota(jnp.int32, both.shape, 1)
    pair = jnp.where(lane < HEAD_DIM, turn(both, c, s), both).astype(BF16)
    kv[...] = pair

    @pl.when(step == 0)
    def _():
        low[:128] = pair[:128]
        low[128:144] = pool_in[:16, :128]
        low[144:160] = pool_in[:16, 128:]

    @pl.when(step == pl.num_programs(0) - 1)
    def _():
        high[:128] = pair[TILE - 128 :]
        high[128:144] = pool_in[TILE - 16 :, :128]
        high[144:160] = pool_in[TILE - 16 :, 128:]


def second_projection(normed, w3, acc, cos, sin):
    whole = pl.BlockSpec((NZ * BLK, IN_W), lambda i: (0, 0))
    rows = lambda w: pl.BlockSpec((TILE, w), lambda i: (i, 0))
    rim = pl.BlockSpec((160, 128), lambda i: (0, 0))
    return pl.pallas_call(
        second_kernel,
        grid=(ROWS // TILE,),
        in_specs=[line_spec(2), whole, rows(IN_W), rows(128), rows(128)],
        out_specs=[rows(POOL_W), rows(Q_W), rows(KV_W), rim, rim],
        out_shape=[
            jax.ShapeDtypeStruct((ROWS, POOL_W), BF16),
            jax.ShapeDtypeStruct((ROWS, Q_W), BF16),
            jax.ShapeDtypeStruct((ROWS, KV_W), BF16),
            jax.ShapeDtypeStruct((160, 128), BF16),
            jax.ShapeDtypeStruct((160, 128), BF16),
        ],
        compiler_params=GRID_PARAMS,
        name="project_second",
    )(normed, w3, acc, cos, sin)


def rotary_rows(offset):
    lane = jnp.arange(128, dtype=jnp.int32)
    inverse = rotary_base ** (-jnp.arange(16, dtype=F32) / 16)
    inverse = jnp.tile(inverse, 8)
    positions = offset + jnp.arange(ROWS, dtype=jnp.int32)
    row_pos = (positions // GRID_W).astype(F32)
    col_pos = (positions % GRID_W).astype(F32)
    by_row = ((lane // 32) % 2 == 0)[None, :]
    angles = jnp.where(by_row, row_pos[:, None], col_pos[:, None]) * inverse
    sine = jnp.sin(angles)
    return jnp.cos(angles), jnp.where(((lane // 16) % 2 == 0)[None, :], -sine, sine)


def attend(q, key_t, values, mask, sink):
    lane = lax.broadcasted_iota(jnp.int32, (BLK, 128), 1)
    row = lax.broadcasted_iota(jnp.int32, (2 * BLK, 1), 0)
    none = jnp.zeros((BLK, 128), BF16)
    outs = []
    for p in range(GROUP // 2):
        pair = q[:, p * 128 : (p + 1) * 128]
        both = jnp.concatenate(
            [jnp.where(lane < 64, pair, none), jnp.where(lane < 64, none, pair)], axis=0
        )
        scores = dot(both, key_t) + mask
        sinks = jnp.where(row < BLK, sink[2 * p], sink[2 * p + 1])
        highest = jnp.maximum(jnp.max(scores, axis=-1, keepdims=True), sinks)
        expo = jnp.exp(scores - highest)
        denominator = jnp.sum(expo, axis=-1, keepdims=True) + jnp.exp(sinks - highest)
        weights = (expo * (1.0 / denominator)).astype(BF16)
        out = dot(weights, values)
        outs.append(jnp.where(lane < 64, out[:BLK], out[BLK:]).astype(BF16))
    return jnp.concatenate(outs, axis=1)


def twice_keys(kv):
    turned = kv.astype(F32).T
    return jnp.concatenate([turned[:64], turned[:64]], axis=0).astype(BF16)


def twice_values(kv):
    wide = kv.astype(F32)
    lane = lax.broadcasted_iota(jnp.int32, wide.shape, 1)
    return jnp.where(lane < 64, pltpu.roll(wide, 64, 1), wide).astype(BF16)


def band():
    shape = (2 * BLK, 3 * BLK)
    i = lax.broadcasted_iota(jnp.int32, shape, 0) % BLK
    j = lax.broadcasted_iota(jnp.int32, shape, 1)
    return jnp.where((j >= i) & (j <= i + 2 * WINDOW), 0.0, masked_score)


def inner_kernel(sink, query, kv, act, key_t, values, mask):
    mask[...] = band()
    for k in range(ROWS // BLK):
        at = slice(k * BLK, (k + 1) * BLK)
        key_t[:, at] = twice_keys(kv[at, :])
        values[at, :] = twice_values(kv[at, :])

    def block(b, carry):
        start = pl.multiple_of(b * BLK, BLK)
        before = pl.multiple_of(start - BLK, BLK)
        act[pl.ds(start, BLK), 256:] = attend(
            query[pl.ds(start, BLK), :],
            key_t[:, pl.ds(before, 3 * BLK)],
            values[pl.ds(before, 3 * BLK), :],
            mask[...],
            sink,
        )
        return carry

    lax.fori_loop(1, ROWS // BLK - 1, block, 0)


def inner_mixer(sink, query, kv):
    return pl.pallas_call(
        inner_kernel,
        in_specs=[smem(), vmem(), vmem()],
        out_specs=vmem(),
        out_shape=jax.ShapeDtypeStruct((ROWS, 512), BF16),
        scratch_shapes=[
            pltpu.VMEM((128, ROWS), BF16),
            pltpu.VMEM((ROWS, 128), BF16),
            pltpu.VMEM((2 * BLK, 3 * BLK), F32),
        ],
        compiler_params=PARAMS,
        name="inner_mixer",
    )(sink, query, kv)


def rim_kernel(place, sink, query, kv, pool, low, high, weight, scale, inner, act, poolx):
    offset, tp = place[4], place[5]
    act[BLK : ROWS - BLK, 256:] = inner[BLK : ROWS - BLK, 256:]
    last = ROWS - BLK
    lane = lax.broadcasted_iota(jnp.int32, (1, 3 * BLK), 1)
    for start, keys in (
        (0, jnp.concatenate([high[:128], kv[: 2 * BLK]], axis=0)),
        (last, jnp.concatenate([kv[last - BLK :], low[:128]], axis=0)),
    ):
        key_pos = offset + start - WINDOW + lane
        edge = jnp.where((key_pos >= 0) & (key_pos < TOTAL), 0.0, masked_score)
        act[start : start + BLK, 256:] = attend(
            query[start : start + BLK, :],
            twice_keys(keys),
            twice_values(keys),
            band() + edge,
            sink,
        )

    poolx[:8, :128] = high[136:144].astype(F32)
    poolx[:8, 128:] = high[152:160].astype(F32)
    poolx[8 : 8 + ROWS] = pool[...].astype(F32)
    poolx[8 + ROWS :, :128] = low[128:136].astype(F32)
    poolx[8 + ROWS :, 128:] = low[144:152].astype(F32)
    level = lax.rem(tp, 4)
    half_width = lax.shift_left(jnp.int32(1), level)

    def block(b, carry):
        start = pl.multiple_of(b * BLK, BLK)
        x = poolx[pl.ds(start, BLK + 2 * REACH), :]
        n = BLK + 2 * REACH
        a1 = x + pltpu.roll(x, n - 1, 0)
        a2 = a1 + pltpu.roll(a1, n - 2, 0)
        a3 = a2 + pltpu.roll(a2, n - 4, 0)
        a4 = a3 + pltpu.roll(a3, n - 8, 0)
        window_sum = jnp.where(
            level == 0,
            a1[7 : 7 + BLK],
            jnp.where(
                level == 1, a2[6 : 6 + BLK], jnp.where(level == 2, a3[4 : 4 + BLK], a4[:BLK])
            ),
        )
        t = offset + start + lax.broadcasted_iota(jnp.int32, (BLK, 1), 0)
        counts = jnp.minimum(t + half_width, TOTAL) - jnp.maximum(t - half_width, 0)
        pooled = (window_sum / counts.astype(F32) - x[8 : 8 + BLK]).astype(BF16)
        mixing = dot(pooled, weight[...])
        act[pl.ds(start, BLK), :256] = (mixing * scale[...]).astype(BF16)
        return carry

    lax.fori_loop(0, ROWS // BLK, block, 0)


def rim_mixer(place, sink, query, kv, pool, low, high, weight, scale, inner):
    return pl.pallas_call(
        rim_kernel,
        in_specs=[smem(), smem()] + [vmem()] * 8,
        out_specs=vmem(),
        out_shape=jax.ShapeDtypeStruct((ROWS, 512), BF16),
        scratch_shapes=[pltpu.VMEM((ROWS + 2 * REACH, POOL_W), F32)],
        compiler_params=PARAMS,
        name="rim_mixer",
    )(place, sink, query, kv, pool, low, high, weight, scale.reshape(1, POOL_W), inner)


def out_kernel(steps, place, act, *refs):
    pieces, outs = refs[:NZ], refs[NZ:]
    z, y, x, c = place[0], place[1], place[2], place[3]
    blocks = []
    for step in steps:
        chip = lax.rem(x + step, NX)
        for core in (c, 1 - c):
            blocks.append(act[pl.ds(pl.multiple_of((chip * 2 + core) * BLK, BLK), BLK), :])
    rows = jnp.concatenate(blocks, axis=0)
    for q in range(NZ):
        o = dot(rows, pieces[q][...]).astype(BF16)
        zz = lax.rem(z - jnp.where(c == 0, q, -q) + NZ, NZ)
        for k in range(NY):
            yy = lax.rem(y - k + NY, NY)
            at = pl.ds(pl.multiple_of((zz * NY + yy) * BLK, BLK), BLK)
            for n, out in enumerate(outs):
                out[:, at] = o[n * BLK : (n + 1) * BLK, k * BLK : (k + 1) * BLK]


def out_chunk(steps, place, act, pieces):
    return pl.pallas_call(
        functools.partial(out_kernel, steps),
        in_specs=[smem()] + [vmem()] * (1 + NZ),
        out_specs=[vmem()] * (2 * len(steps)),
        out_shape=[jax.ShapeDtypeStruct((BLK, D), BF16)] * (2 * len(steps)),
        compiler_params=PARAMS,
    )(place, act, *pieces)


def total(*parts):
    return sum(p.astype(F32) for p in parts)


def added(*parts):
    return total(*parts).astype(BF16)


def shards(
    tokens,
    norm_gain,
    pool_in_weight,
    query_weight,
    key_weight,
    value_weight,
    pool_weight,
    pool_scale,
    sink_logit,
    out_pool_weight,
    out_attn_weight,
):
    z, y, x, c = (lax.axis_index(a) for a in ("z", "y", "x", "c"))
    offset = (z * NY + y) * ROWS
    place = jnp.stack([z, y, x, c, offset, x * NC + c]).astype(jnp.int32)

    swap = lambda a: shift(a, "c", NC, 1)

    flat = []
    for t in both_ways(tokens, "x", NX):
        flat += [t, swap(t)]

    w_in = jnp.concatenate([pool_in_weight, query_weight, key_weight, value_weight], axis=1)
    quarter = packed(both_ways(w_in, "z", NZ))
    w = both_ways(quarter, "y", NY)

    w_out = jnp.concatenate([out_pool_weight, out_attn_weight], axis=0)
    ys = [w_out] + [shift(w_out, "y", NY, k) for k in (1, 2, 3)]
    pieces = both_ways(jnp.concatenate(ys, axis=1), "z", NZ)

    cos, sin = rotary_rows(offset)
    normed = normed_rows(place, flat, norm_gain)
    acc = first_projection(normed, w[0], w[1], w[3])
    pool, query, kv, low, high = second_projection(normed, w[2], acc, cos, sin)

    count = NZ * NY
    forward = [(i, i + 1) for i in range(count - 1)]
    backward = [(i + 1, i) for i in range(count - 1)]
    from_before = lax.ppermute(high, ("z", "y"), forward)
    from_after = lax.ppermute(low, ("z", "y"), backward)
    inner = inner_mixer(sink_logit, query, kv)
    act = rim_mixer(
        place,
        sink_logit,
        query,
        kv,
        pool,
        from_after,
        from_before,
        pool_weight[0],
        pool_scale,
        inner,
    )

    half = D // 2
    keep2, send2 = out_chunk((2,), place, act, pieces)
    part2 = swap(send2)
    a = shift(added(keep2[:, :half], part2[:, :half]), "x", NX, 1)
    b = shift(added(keep2[:, half:], part2[:, half:]), "x", NX, -1)
    keep1, send1, keep3, send3 = out_chunk((1, 3), place, act, pieces)
    part1 = swap(send1)
    part3 = swap(send3)
    early = lax.optimization_barrier((keep1, part1))
    right_high = shift(added(*[v[:, half:] for v in early]), "x", NX, 1)
    early = lax.optimization_barrier((keep3, part3))
    sum3 = added(*[v[:, :half] for v in early])
    left_low = shift(sum3, "x", NX, -1)
    right_low = shift(added(keep1[:, :half], part1[:, :half], a), "x", NX, 1)
    left_high = shift(added(keep3[:, half:], part3[:, half:], b), "x", NX, -1)
    keep0, send0 = out_chunk((0,), place, act, pieces)
    part0 = swap(send0)
    low = total(keep0[:, :half], part0[:, :half], left_low)
    high = total(keep0[:, half:], part0[:, half:], right_high)
    low, high = lax.optimization_barrier((low, high))
    return jnp.concatenate([added(low, right_low), added(high, left_high)], axis=1)


def solution(mesh):
    finer = Mesh(mesh.devices.reshape(NZ, NY, NX, NC), ("z", "y", "x", "c"))
    sp, tp = ("z", "y"), ("x", "c")
    return jax.shard_map(
        shards,
        mesh=finer,
        in_specs=(
            P(sp, tp),
            P(),
            P(sp, tp),
            P(sp, tp),
            P(sp, tp),
            P(sp, tp),
            P(tp, None, None),
            P(tp),
            P(tp),
            P(tp, sp),
            P(tp, sp),
        ),
        out_specs=P(sp + tp, None),
        check_vma=False,
    )
```

```python
import functools

import jax
import jax.numpy as jnp
from jax import lax
from jax.experimental import pallas as pl
from jax.experimental.pallas import tpu as pltpu
from jax.sharding import Mesh
from jax.sharding import PartitionSpec as P


NZ, NY, NX, NC = 8, 4, 4, 2
HEAD_DIM = 64
GROUP = 4
WINDOW = 128
GRID_W = 64
REACH = 8
ROWS = 1024
TOTAL = ROWS * NZ * NY
BLK = 128
POOL_W = 256
Q_W = 256
KV_W = 128
IN_W = POOL_W + Q_W + KV_W
D = 4096
epsilon = 1e-06
rotary_base = 10000.0
masked_score = -1e30
F32 = jnp.float32
BF16 = jnp.bfloat16


def shift(array, axis, size, step):
    return lax.ppermute(array, axis, [(i, (i + step) % size) for i in range(size)])


def dot(a, b):
    return jnp.dot(a, b, preferred_element_type=F32)


def vmem():
    return pl.BlockSpec(memory_space=pltpu.VMEM)


def smem():
    return pl.BlockSpec(memory_space=pltpu.SMEM)


PARAMS = pltpu.CompilerParams(vmem_limit_bytes=20 * 1024 * 1024)
SMALL = pltpu.CompilerParams(vmem_limit_bytes=8 * 1024 * 1024)
GRID_PARAMS = pltpu.CompilerParams(
    dimension_semantics=("arbitrary",), vmem_limit_bytes=20 * 1024 * 1024
)


def one_way(array, axis, step):
    size = {"x": NX, "y": NY, "z": NZ}[axis]
    pairs = []
    for i in range(size):
        for c, sign in enumerate((1, -1)):
            pairs.append((i * NC + c, (i + sign * step) % size * NC + c))
    return lax.ppermute(array, (axis, "c"), pairs)


def both_ways(block, axis, size):
    out = {0: block}
    ahead = behind = block
    for k in range(1, size // 2):
        ahead = out[k] = one_way(ahead, axis, 1)
        behind = out[size - k] = one_way(behind, axis, -1)
    out[size // 2] = one_way(ahead, axis, 1)
    return [out[k] for k in range(size)]


def pack_kernel(*refs):
    pieces, out = refs[:-1], refs[-1]
    rows = pieces[0].shape[0]
    for k, piece in enumerate(pieces):
        out[k * rows : (k + 1) * rows, :] = piece[...]


def packed(pieces):
    rows, width = pieces[0].shape
    return pl.pallas_call(
        pack_kernel,
        in_specs=[vmem()] * len(pieces),
        out_specs=vmem(),
        out_shape=jax.ShapeDtypeStruct((rows * len(pieces), width), BF16),
        compiler_params=PARAMS,
        name="pack",
    )(*pieces)


def input_kernel(pool, query, key_t, value_t, out, both, sems):
    copies = [
        pltpu.make_async_copy(pool, out.at[:, :POOL_W], sems.at[0]),
        pltpu.make_async_copy(query, out.at[:, POOL_W : POOL_W + Q_W], sems.at[1]),
        pltpu.make_async_copy(key_t, both.at[:HEAD_DIM], sems.at[2]),
        pltpu.make_async_copy(value_t, both.at[HEAD_DIM:], sems.at[3]),
    ]
    for copy in copies:
        copy.start()
    for copy in copies:
        copy.wait()
    out[:, POOL_W + Q_W :] = both[...].astype(F32).T.astype(BF16)


def input_block(pool, query, key, value):
    return pl.pallas_call(
        input_kernel,
        in_specs=[pl.BlockSpec(memory_space=pl.ANY)] * 4,
        out_specs=vmem(),
        out_shape=jax.ShapeDtypeStruct((BLK, IN_W), BF16),
        scratch_shapes=[pltpu.VMEM((KV_W, BLK), BF16), pltpu.SemaphoreType.DMA((4,))],
        compiler_params=SMALL,
        name="ji",
    )(pool, query, key.T, value.T)


def stack_kernel(a, b, out, sems):
    n = a.shape[0]
    copies = [
        pltpu.make_async_copy(a, out.at[:n], sems.at[0]),
        pltpu.make_async_copy(b, out.at[n:], sems.at[1]),
    ]
    for copy in copies:
        copy.start()
    for copy in copies:
        copy.wait()


def stacked(a, b):
    return pl.pallas_call(
        stack_kernel,
        in_specs=[pl.BlockSpec(memory_space=pl.ANY)] * 2,
        out_specs=vmem(),
        out_shape=jax.ShapeDtypeStruct((a.shape[0] + b.shape[0], a.shape[1]), BF16),
        scratch_shapes=[pltpu.SemaphoreType.DMA((2,))],
        compiler_params=SMALL,
        name="j0",
    )(a, b)


def join_kernel(a, b, out):
    n = a.shape[1]
    out[:, :n] = a[...]
    out[:, n:] = b[...]


def joined(a, b):
    return pl.pallas_call(
        join_kernel,
        in_specs=[vmem()] * 2,
        out_specs=vmem(),
        out_shape=jax.ShapeDtypeStruct((a.shape[0], a.shape[1] + b.shape[1]), BF16),
        compiler_params=SMALL,
    )(a, b)


def signed(c, value, size):
    return lax.rem(jnp.where(c == 0, value, -value) + 2 * size, size)


def norm_kernel(place, *refs):
    shards, (gain, out) = refs[:8], refs[8:]
    z, y, x, c = place[0], place[1], place[2], place[3]


    def some(r, carry):
        rows = pl.ds(pl.multiple_of(r * 32, 32), 32)
        values = [shard[rows, :].astype(F32) for shard in shards]
        square = sum(v * v for v in values)
        scale = lax.rsqrt(jnp.sum(square, axis=-1, keepdims=True) * (1.0 / D) + epsilon)
        for k, v in enumerate(values):
            core = c if k % 2 == 0 else 1 - c
            chip = lax.rem(x - jnp.where(core == 0, k // 2, -(k // 2)) + NX, NX)
            zz = chip * NC + core
            g = gain[:, pl.ds(pl.multiple_of(zz * 512, 512), 512)]
            n = ((v * scale) * g).astype(BF16)
            slot = signed(c, z - zz, NZ)
            for yy in range(NY):
                line = signed(c, y - yy, NY)
                out[line, rows, pl.ds(pl.multiple_of(slot * BLK, BLK), BLK)] = n[
                    :, yy * BLK : (yy + 1) * BLK
                ]
        return carry

    lax.fori_loop(0, BLK // 32, some, 0)


def normed_rows(place, shards, gain):
    block = pl.BlockSpec((BLK, 512), lambda i: (i, 0))
    return pl.pallas_call(
        norm_kernel,
        grid=(ROWS // BLK,),
        in_specs=[smem()] + [block] * 8 + [pl.BlockSpec((1, D), lambda i: (0, 0))],
        out_specs=pl.BlockSpec((NY, BLK, NZ * BLK), lambda i: (0, i, 0)),
        out_shape=jax.ShapeDtypeStruct((NY, ROWS, NZ * BLK), BF16),
        compiler_params=GRID_PARAMS,
        name="norm",
    )(place, *shards, gain.reshape(1, D))


def first_kernel(n0, n1, n2, w0, w1, w2, acc):
    acc[...] = dot(n0[0], w0[...]) + dot(n1[0], w1[...]) + dot(n2[0], w2[...])


TILE = 256


def line_spec(line):
    return pl.BlockSpec((1, TILE, NZ * BLK), lambda i: (line, i, 0))


def first_projection(normed, w0, w1, w2):
    whole = pl.BlockSpec((NZ * BLK, IN_W), lambda i: (0, 0))
    return pl.pallas_call(
        first_kernel,
        grid=(ROWS // TILE,),
        in_specs=[line_spec(0), line_spec(1), line_spec(3), whole, whole, whole],
        out_specs=pl.BlockSpec((TILE, IN_W), lambda i: (i, 0)),
        out_shape=jax.ShapeDtypeStruct((ROWS, IN_W), F32),
        compiler_params=GRID_PARAMS,
        name="project_first",
    )(normed, normed, normed, w0, w1, w2)


def turn(v, cosine, sine):
    lane = lax.broadcasted_iota(jnp.int32, v.shape, 1)
    even = (lane // 16) % 2 == 0
    other = jnp.where(even, pltpu.roll(v, 112, 1), pltpu.roll(v, 16, 1))
    return v * cosine + other * sine


def second_kernel(n3, w3, acc, cos, sin, pool, query, kv, low, high):
    step = pl.program_id(0)
    raw = acc[...] + dot(n3[0], w3[...])
    pool_in = raw[:, :POOL_W].astype(BF16)
    pool[...] = pool_in
    c, s = cos[...], sin[...]
    factor = jnp.asarray(HEAD_DIM**-0.5, BF16)
    query[:, :128] = turn(raw[:, 256:384], c, s).astype(BF16) * factor
    query[:, 128:] = turn(raw[:, 384:512], c, s).astype(BF16) * factor
    both = raw[:, 512:640]
    lane = lax.broadcasted_iota(jnp.int32, both.shape, 1)
    pair = jnp.where(lane < HEAD_DIM, turn(both, c, s), both).astype(BF16)
    kv[...] = pair

    @pl.when(step == 0)
    def _():
        low[:128] = pair[:128]
        low[128:144] = pool_in[:16, :128]
        low[144:160] = pool_in[:16, 128:]

    @pl.when(step == pl.num_programs(0) - 1)
    def _():
        high[:128] = pair[TILE - 128 :]
        high[128:144] = pool_in[TILE - 16 :, :128]
        high[144:160] = pool_in[TILE - 16 :, 128:]


def second_projection(normed, w3, acc, cos, sin):
    whole = pl.BlockSpec((NZ * BLK, IN_W), lambda i: (0, 0))
    rows = lambda w: pl.BlockSpec((TILE, w), lambda i: (i, 0))
    rim = pl.BlockSpec((160, 128), lambda i: (0, 0))
    return pl.pallas_call(
        second_kernel,
        grid=(ROWS // TILE,),
        in_specs=[line_spec(2), whole, rows(IN_W), rows(128), rows(128)],
        out_specs=[rows(POOL_W), rows(Q_W), rows(KV_W), rim, rim],
        out_shape=[
            jax.ShapeDtypeStruct((ROWS, POOL_W), BF16),
            jax.ShapeDtypeStruct((ROWS, Q_W), BF16),
            jax.ShapeDtypeStruct((ROWS, KV_W), BF16),
            jax.ShapeDtypeStruct((160, 128), BF16),
            jax.ShapeDtypeStruct((160, 128), BF16),
        ],
        compiler_params=GRID_PARAMS,
        name="project_second",
    )(normed, w3, acc, cos, sin)


def rotary_rows(offset):
    lane = jnp.arange(128, dtype=jnp.int32)
    inverse = rotary_base ** (-jnp.arange(16, dtype=F32) / 16)
    inverse = jnp.tile(inverse, 8)
    positions = offset + jnp.arange(ROWS, dtype=jnp.int32)
    row_pos = (positions // GRID_W).astype(F32)
    col_pos = (positions % GRID_W).astype(F32)
    by_row = ((lane // 32) % 2 == 0)[None, :]
    angles = jnp.where(by_row, row_pos[:, None], col_pos[:, None]) * inverse
    sine = jnp.sin(angles)
    return jnp.cos(angles), jnp.where(((lane // 16) % 2 == 0)[None, :], -sine, sine)


def attend(q, key_t, values, mask, sink):
    lane = lax.broadcasted_iota(jnp.int32, (BLK, 128), 1)
    row = lax.broadcasted_iota(jnp.int32, (2 * BLK, 1), 0)
    none = jnp.zeros((BLK, 128), BF16)
    outs = []
    for p in range(GROUP // 2):
        pair = q[:, p * 128 : (p + 1) * 128]
        both = jnp.concatenate(
            [jnp.where(lane < 64, pair, none), jnp.where(lane < 64, none, pair)], axis=0
        )
        scores = dot(both, key_t) + mask
        sinks = jnp.where(row < BLK, sink[2 * p], sink[2 * p + 1])
        highest = jnp.maximum(jnp.max(scores, axis=-1, keepdims=True), sinks)
        expo = jnp.exp(scores - highest)
        denominator = jnp.sum(expo, axis=-1, keepdims=True) + jnp.exp(sinks - highest)
        weights = (expo * (1.0 / denominator)).astype(BF16)
        out = dot(weights, values)
        outs.append(jnp.where(lane < 64, out[:BLK], out[BLK:]).astype(BF16))
    return jnp.concatenate(outs, axis=1)


def twice_keys(kv):
    turned = kv.astype(F32).T
    return jnp.concatenate([turned[:64], turned[:64]], axis=0).astype(BF16)


def twice_values(kv):
    wide = kv.astype(F32)
    lane = lax.broadcasted_iota(jnp.int32, wide.shape, 1)
    return jnp.where(lane < 64, pltpu.roll(wide, 64, 1), wide).astype(BF16)


def band():
    shape = (2 * BLK, 3 * BLK)
    i = lax.broadcasted_iota(jnp.int32, shape, 0) % BLK
    j = lax.broadcasted_iota(jnp.int32, shape, 1)
    return jnp.where((j >= i) & (j <= i + 2 * WINDOW), 0.0, masked_score)


def inner_kernel(sink, query, kv, act, key_t, values, mask):
    mask[...] = band()
    for k in range(ROWS // BLK):
        at = slice(k * BLK, (k + 1) * BLK)
        key_t[:, at] = twice_keys(kv[at, :])
        values[at, :] = twice_values(kv[at, :])

    def block(b, carry):
        start = pl.multiple_of(b * BLK, BLK)
        before = pl.multiple_of(start - BLK, BLK)
        act[pl.ds(start, BLK), 256:] = attend(
            query[pl.ds(start, BLK), :],
            key_t[:, pl.ds(before, 3 * BLK)],
            values[pl.ds(before, 3 * BLK), :],
            mask[...],
            sink,
        )
        return carry

    lax.fori_loop(1, ROWS // BLK - 1, block, 0)


def inner_mixer(sink, query, kv):
    return pl.pallas_call(
        inner_kernel,
        in_specs=[smem(), vmem(), vmem()],
        out_specs=vmem(),
        out_shape=jax.ShapeDtypeStruct((ROWS, 512), BF16),
        scratch_shapes=[
            pltpu.VMEM((128, ROWS), BF16),
            pltpu.VMEM((ROWS, 128), BF16),
            pltpu.VMEM((2 * BLK, 3 * BLK), F32),
        ],
        compiler_params=PARAMS,
        name="inner_mixer",
    )(sink, query, kv)


def rim_kernel(place, sink, query, kv, pool, low, high, weight, scale, inner, act, poolx, ends):
    offset, tp = place[4], place[5]
    act[BLK : ROWS - BLK, 256:] = inner[BLK : ROWS - BLK, 256:]
    last = ROWS - BLK
    lane = lax.broadcasted_iota(jnp.int32, (1, 3 * BLK), 1)
    span = 3 * BLK
    ends[: BLK] = high[:BLK]
    ends[BLK:span] = kv[: 2 * BLK]
    ends[span : span + 2 * BLK] = kv[last - BLK :]
    ends[span + 2 * BLK :] = low[:BLK]

    def end(e, carry):
        start = pl.multiple_of(e * last, BLK)
        keys = ends[pl.ds(pl.multiple_of(e * span, BLK), span), :]
        key_pos = offset + start - WINDOW + lane
        edge = jnp.where((key_pos >= 0) & (key_pos < TOTAL), 0.0, masked_score)
        act[pl.ds(start, BLK), 256:] = attend(
            query[pl.ds(start, BLK), :],
            twice_keys(keys),
            twice_values(keys),
            band() + edge,
            sink,
        )
        return carry

    lax.fori_loop(0, 2, end, 0)

    poolx[:8, :128] = high[136:144].astype(F32)
    poolx[:8, 128:] = high[152:160].astype(F32)
    poolx[8 : 8 + ROWS] = pool[...].astype(F32)
    poolx[8 + ROWS :, :128] = low[128:136].astype(F32)
    poolx[8 + ROWS :, 128:] = low[144:152].astype(F32)
    level = lax.rem(tp, 4)
    half_width = lax.shift_left(jnp.int32(1), level)

    def block(b, carry):
        start = pl.multiple_of(b * BLK, BLK)
        x = poolx[pl.ds(start, BLK + 2 * REACH), :]
        n = BLK + 2 * REACH
        a1 = x + pltpu.roll(x, n - 1, 0)
        a2 = a1 + pltpu.roll(a1, n - 2, 0)
        a3 = a2 + pltpu.roll(a2, n - 4, 0)
        a4 = a3 + pltpu.roll(a3, n - 8, 0)
        window_sum = jnp.where(
            level == 0,
            a1[7 : 7 + BLK],
            jnp.where(
                level == 1, a2[6 : 6 + BLK], jnp.where(level == 2, a3[4 : 4 + BLK], a4[:BLK])
            ),
        )
        t = offset + start + lax.broadcasted_iota(jnp.int32, (BLK, 1), 0)
        counts = jnp.minimum(t + half_width, TOTAL) - jnp.maximum(t - half_width, 0)
        pooled = (window_sum / counts.astype(F32) - x[8 : 8 + BLK]).astype(BF16)
        mixing = dot(pooled, weight[...])
        act[pl.ds(start, BLK), :256] = (mixing * scale[...]).astype(BF16)
        return carry

    lax.fori_loop(0, ROWS // BLK, block, 0)


def rim_mixer(place, sink, query, kv, pool, low, high, weight, scale, inner):
    return pl.pallas_call(
        rim_kernel,
        in_specs=[smem(), smem()] + [vmem()] * 8,
        out_specs=vmem(),
        out_shape=jax.ShapeDtypeStruct((ROWS, 512), BF16),
        scratch_shapes=[
            pltpu.VMEM((ROWS + 2 * REACH, POOL_W), F32),
            pltpu.VMEM((6 * BLK, KV_W), BF16),
        ],
        compiler_params=PARAMS,
        name="rim_mixer",
    )(place, sink, query, kv, pool, low, high, weight, scale.reshape(1, POOL_W), inner)


def out_kernel(steps, place, act, *refs):
    pieces, (keep, send) = refs[:NZ], refs[NZ:]
    z, y, x, c = place[0], place[1], place[2], place[3]
    blocks = []
    for core in (c, 1 - c):
        for step in steps:
            chip = lax.rem(x + step, NX)
            blocks.append(act[pl.ds(pl.multiple_of((chip * 2 + core) * BLK, BLK), BLK), :])
    rows = jnp.concatenate(blocks, axis=0)
    n = len(steps) * BLK
    for q in range(NZ):
        o = dot(rows, pieces[q][...]).astype(BF16)
        zz = lax.rem(z - jnp.where(c == 0, q, -q) + NZ, NZ)
        for t, k in enumerate((0, 2, 1, 3)):
            yy = lax.rem(y - jnp.where(c == 0, k, -k) + NY, NY)
            at = pl.ds(pl.multiple_of((zz * NY + yy) * BLK, BLK), BLK)
            keep[:, at] = o[:n, t * BLK : (t + 1) * BLK]
            send[:, at] = o[n:, t * BLK : (t + 1) * BLK]


def out_chunk(steps, place, act, pieces):
    shape = jax.ShapeDtypeStruct((len(steps) * BLK, D), BF16)
    return pl.pallas_call(
        functools.partial(out_kernel, steps),
        in_specs=[smem()] + [vmem()] * (1 + NZ),
        out_specs=[vmem()] * 2,
        out_shape=[shape] * 2,
        compiler_params=PARAMS,
    )(place, act, *pieces)


def total(*parts):
    return sum(p.astype(F32) for p in parts)


def added(*parts):
    return total(*parts).astype(BF16)


def shards(
    tokens,
    norm_gain,
    pool_in_weight,
    query_weight,
    key_weight,
    value_weight,
    pool_weight,
    pool_scale,
    sink_logit,
    out_pool_weight,
    out_attn_weight,
):
    z, y, x, c = (lax.axis_index(a) for a in ("z", "y", "x", "c"))
    offset = (z * NY + y) * ROWS
    place = jnp.stack([z, y, x, c, offset, x * NC + c]).astype(jnp.int32)

    swap = lambda a: shift(a, "c", NC, 1)

    flat = []
    for t in both_ways(tokens, "x", NX):
        flat += [t, swap(t)]

    w_in = input_block(pool_in_weight, query_weight, key_weight, value_weight)
    quarter = packed(both_ways(w_in, "z", NZ))
    w = both_ways(quarter, "y", NY)

    unit = stacked(out_pool_weight, out_attn_weight)
    unit = joined(unit, shift(unit, "y", NY, 2))
    unit = joined(unit, one_way(unit, "y", 1))
    pieces = both_ways(unit, "z", NZ)

    cos, sin = rotary_rows(offset)
    normed = normed_rows(place, flat, norm_gain)
    acc = first_projection(normed, w[0], w[1], w[3])
    pool, query, kv, low, high = second_projection(normed, w[2], acc, cos, sin)

    count = NZ * NY
    forward = [(i, i + 1) for i in range(count - 1)]
    backward = [(i + 1, i) for i in range(count - 1)]
    from_before = lax.ppermute(high, ("z", "y"), forward)
    from_after = lax.ppermute(low, ("z", "y"), backward)
    inner = inner_mixer(sink_logit, query, kv)
    act = rim_mixer(
        place,
        sink_logit,
        query,
        kv,
        pool,
        from_after,
        from_before,
        pool_weight[0],
        pool_scale,
        inner,
    )

    half = D // 2
    keep2, send2 = out_chunk((2,), place, act, pieces)
    part2 = swap(send2)
    a = shift(added(keep2[:, :half], part2[:, :half]), "x", NX, 1)
    b = shift(added(keep2[:, half:], part2[:, half:]), "x", NX, -1)
    keeps, sends = out_chunk((1, 3), place, act, pieces)
    parts = swap(sends)
    early = lax.optimization_barrier((keeps, parts))
    right_high = shift(added(*[v[:BLK, half:] for v in early]), "x", NX, 1)
    early = lax.optimization_barrier((keeps, parts))
    left_low = shift(added(*[v[BLK:, :half] for v in early]), "x", NX, -1)
    right_low = shift(added(keeps[:BLK, :half], parts[:BLK, :half], a), "x", NX, 1)
    left_high = shift(added(keeps[BLK:, half:], parts[BLK:, half:], b), "x", NX, -1)
    keep0, send0 = out_chunk((0,), place, act, pieces)
    part0 = swap(send0)
    low = total(keep0[:, :half], part0[:, :half], left_low)
    high = total(keep0[:, half:], part0[:, half:], right_high)
    low, high = lax.optimization_barrier((low, high))
    return jnp.concatenate([added(low, right_low), added(high, left_high)], axis=1)


def solution(mesh):
    finer = Mesh(mesh.devices.reshape(NZ, NY, NX, NC), ("z", "y", "x", "c"))
    sp, tp = ("z", "y"), ("x", "c")
    return jax.shard_map(
        shards,
        mesh=finer,
        in_specs=(
            P(sp, tp),
            P(),
            P(sp, tp),
            P(sp, tp),
            P(sp, tp),
            P(sp, tp),
            P(tp, None, None),
            P(tp),
            P(tp),
            P(tp, sp),
            P(tp, sp),
        ),
        out_specs=P(sp + tp, None),
        check_vma=False,
    )
```

```python
import functools

import jax
import jax.numpy as jnp
from jax import lax
from jax.experimental import pallas as pl
from jax.experimental.pallas import tpu as pltpu
from jax.sharding import Mesh
from jax.sharding import PartitionSpec as P


NZ, NY, NX, NC = 8, 4, 4, 2
HEAD_DIM = 64
GROUP = 4
WINDOW = 128
GRID_W = 64
REACH = 8
ROWS = 1024
TOTAL = ROWS * NZ * NY
BLK = 128
POOL_W = 256
Q_W = 256
KV_W = 128
IN_W = POOL_W + Q_W + KV_W
D = 4096
epsilon = 1e-06
rotary_base = 10000.0
masked_score = -1e30
F32 = jnp.float32
BF16 = jnp.bfloat16


def shift(array, axis, size, step):
    return lax.ppermute(array, axis, [(i, (i + step) % size) for i in range(size)])


def dot(a, b):
    return jnp.dot(a, b, preferred_element_type=F32)


def vmem():
    return pl.BlockSpec(memory_space=pltpu.VMEM)


def smem():
    return pl.BlockSpec(memory_space=pltpu.SMEM)


PARAMS = pltpu.CompilerParams(vmem_limit_bytes=20 * 1024 * 1024)
SMALL = pltpu.CompilerParams(vmem_limit_bytes=8 * 1024 * 1024)
GRID_PARAMS = pltpu.CompilerParams(
    dimension_semantics=("arbitrary",), vmem_limit_bytes=20 * 1024 * 1024
)


def one_way(array, axis, step):
    size = {"x": NX, "y": NY, "z": NZ}[axis]
    pairs = []
    for i in range(size):
        for c, sign in enumerate((1, -1)):
            pairs.append((i * NC + c, (i + sign * step) % size * NC + c))
    return lax.ppermute(array, (axis, "c"), pairs)


def both_ways(block, axis, size):
    out = {0: block}
    ahead = behind = block
    for k in range(1, size // 2):
        ahead = out[k] = one_way(ahead, axis, 1)
        behind = out[size - k] = one_way(behind, axis, -1)
    out[size // 2] = one_way(ahead, axis, 1)
    return [out[k] for k in range(size)]


def pack_kernel(*refs):
    pieces, out = refs[:-1], refs[-1]
    rows = pieces[0].shape[0]
    for k, piece in enumerate(pieces):
        out[k * rows : (k + 1) * rows, :] = piece[...]


def packed(pieces):
    rows, width = pieces[0].shape
    return pl.pallas_call(
        pack_kernel,
        in_specs=[vmem()] * len(pieces),
        out_specs=vmem(),
        out_shape=jax.ShapeDtypeStruct((rows * len(pieces), width), BF16),
        compiler_params=PARAMS,
        name="pack",
    )(*pieces)


def input_kernel(pool, query, key_t, value_t, out, both, sems):
    copies = [
        pltpu.make_async_copy(pool, out.at[:, :POOL_W], sems.at[0]),
        pltpu.make_async_copy(query, out.at[:, POOL_W : POOL_W + Q_W], sems.at[1]),
        pltpu.make_async_copy(key_t, both.at[:HEAD_DIM], sems.at[2]),
        pltpu.make_async_copy(value_t, both.at[HEAD_DIM:], sems.at[3]),
    ]
    for copy in copies:
        copy.start()
    for copy in copies:
        copy.wait()
    out[:, POOL_W + Q_W :] = both[...].astype(F32).T.astype(BF16)


def input_block(pool, query, key, value):
    return pl.pallas_call(
        input_kernel,
        in_specs=[pl.BlockSpec(memory_space=pltpu.HBM)] * 4,
        out_specs=vmem(),
        out_shape=jax.ShapeDtypeStruct((BLK, IN_W), BF16),
        scratch_shapes=[pltpu.VMEM((KV_W, BLK), BF16), pltpu.SemaphoreType.DMA((4,))],
        compiler_params=SMALL,
        name="ji",
    )(pool, query, key.T, value.T)


def stack_kernel(a, b, out, sems):
    n = a.shape[0]
    copies = [
        pltpu.make_async_copy(a, out.at[:n], sems.at[0]),
        pltpu.make_async_copy(b, out.at[n:], sems.at[1]),
    ]
    for copy in copies:
        copy.start()
    for copy in copies:
        copy.wait()


def stacked(a, b):
    return pl.pallas_call(
        stack_kernel,
        in_specs=[pl.BlockSpec(memory_space=pltpu.HBM)] * 2,
        out_specs=vmem(),
        out_shape=jax.ShapeDtypeStruct((a.shape[0] + b.shape[0], a.shape[1]), BF16),
        scratch_shapes=[pltpu.SemaphoreType.DMA((2,))],
        compiler_params=SMALL,
        name="j0",
    )(a, b)


def join_kernel(a, b, out):
    n = a.shape[1]
    out[:, :n] = a[...]
    out[:, n:] = b[...]


def joined(a, b):
    return pl.pallas_call(
        join_kernel,
        in_specs=[vmem()] * 2,
        out_specs=vmem(),
        out_shape=jax.ShapeDtypeStruct((a.shape[0], a.shape[1] + b.shape[1]), BF16),
        compiler_params=SMALL,
    )(a, b)


def signed(c, value, size):
    return lax.rem(jnp.where(c == 0, value, -value) + 2 * size, size)


def norm_kernel(place, *refs):
    shards, (gain, out) = refs[:8], refs[8:]
    z, y, x, c = place[0], place[1], place[2], place[3]


    def some(r, carry):
        rows = pl.ds(pl.multiple_of(r * 32, 32), 32)
        values = [shard[rows, :].astype(F32) for shard in shards]
        square = sum(v * v for v in values)
        scale = lax.rsqrt(jnp.sum(square, axis=-1, keepdims=True) * (1.0 / D) + epsilon)
        for k, v in enumerate(values):
            core = c if k % 2 == 0 else 1 - c
            chip = lax.rem(x - jnp.where(core == 0, k // 2, -(k // 2)) + NX, NX)
            zz = chip * NC + core
            g = gain[:, pl.ds(pl.multiple_of(zz * 512, 512), 512)]
            n = ((v * scale) * g).astype(BF16)
            slot = signed(c, z - zz, NZ)
            for yy in range(NY):
                line = signed(c, y - yy, NY)
                out[line, rows, pl.ds(pl.multiple_of(slot * BLK, BLK), BLK)] = n[
                    :, yy * BLK : (yy + 1) * BLK
                ]
        return carry

    lax.fori_loop(0, ROWS // 32, some, 0)


def normed_rows(place, shards, gain):
    return pl.pallas_call(
        norm_kernel,
        in_specs=[smem()] + [vmem()] * 9,
        out_specs=vmem(),
        out_shape=jax.ShapeDtypeStruct((NY, ROWS, NZ * BLK), BF16),
        compiler_params=PARAMS,
        name="norm",
    )(place, *shards, gain.reshape(1, D))


def first_kernel(n0, n1, n2, w0, w1, w2, acc):
    acc[...] = dot(n0[0], w0[...]) + dot(n1[0], w1[...]) + dot(n2[0], w2[...])


TILE = 256


def line_spec(line):
    return pl.BlockSpec((1, TILE, NZ * BLK), lambda i: (line, i, 0))


def first_projection(normed, w0, w1, w2):
    whole = pl.BlockSpec((NZ * BLK, IN_W), lambda i: (0, 0))
    return pl.pallas_call(
        first_kernel,
        grid=(ROWS // TILE,),
        in_specs=[line_spec(0), line_spec(1), line_spec(3), whole, whole, whole],
        out_specs=pl.BlockSpec((TILE, IN_W), lambda i: (i, 0)),
        out_shape=jax.ShapeDtypeStruct((ROWS, IN_W), F32),
        compiler_params=GRID_PARAMS,
        name="project_first",
    )(normed, normed, normed, w0, w1, w2)


def turn(v, cosine, sine):
    lane = lax.broadcasted_iota(jnp.int32, v.shape, 1)
    even = (lane // 16) % 2 == 0
    other = jnp.where(even, pltpu.roll(v, 112, 1), pltpu.roll(v, 16, 1))
    return v * cosine + other * sine


def second_kernel(n3, w3, acc, cos, sin, pool, query, kv, low, high):
    step = pl.program_id(0)
    raw = acc[...] + dot(n3[0], w3[...])
    pool_in = raw[:, :POOL_W].astype(BF16)
    pool[...] = pool_in
    c, s = cos[...], sin[...]
    factor = jnp.asarray(HEAD_DIM**-0.5, BF16)
    query[:, :128] = turn(raw[:, 256:384], c, s).astype(BF16) * factor
    query[:, 128:] = turn(raw[:, 384:512], c, s).astype(BF16) * factor
    both = raw[:, 512:640]
    lane = lax.broadcasted_iota(jnp.int32, both.shape, 1)
    pair = jnp.where(lane < HEAD_DIM, turn(both, c, s), both).astype(BF16)
    kv[...] = pair

    @pl.when(step == 0)
    def _():
        low[:128] = pair[:128]
        low[128:144] = pool_in[:16, :128]
        low[144:160] = pool_in[:16, 128:]

    @pl.when(step == pl.num_programs(0) - 1)
    def _():
        high[:128] = pair[TILE - 128 :]
        high[128:144] = pool_in[TILE - 16 :, :128]
        high[144:160] = pool_in[TILE - 16 :, 128:]


def second_projection(normed, w3, acc, cos, sin):
    whole = pl.BlockSpec((NZ * BLK, IN_W), lambda i: (0, 0))
    rows = lambda w: pl.BlockSpec((TILE, w), lambda i: (i, 0))
    rim = pl.BlockSpec((160, 128), lambda i: (0, 0))
    return pl.pallas_call(
        second_kernel,
        grid=(ROWS // TILE,),
        in_specs=[line_spec(2), whole, rows(IN_W), rows(128), rows(128)],
        out_specs=[rows(POOL_W), rows(Q_W), rows(KV_W), rim, rim],
        out_shape=[
            jax.ShapeDtypeStruct((ROWS, POOL_W), BF16),
            jax.ShapeDtypeStruct((ROWS, Q_W), BF16),
            jax.ShapeDtypeStruct((ROWS, KV_W), BF16),
            jax.ShapeDtypeStruct((160, 128), BF16),
            jax.ShapeDtypeStruct((160, 128), BF16),
        ],
        compiler_params=GRID_PARAMS,
        name="project_second",
    )(normed, w3, acc, cos, sin)


def rotary_rows(offset):
    lane = jnp.arange(128, dtype=jnp.int32)
    inverse = rotary_base ** (-jnp.arange(16, dtype=F32) / 16)
    inverse = jnp.tile(inverse, 8)
    positions = offset + jnp.arange(ROWS, dtype=jnp.int32)
    row_pos = (positions // GRID_W).astype(F32)
    col_pos = (positions % GRID_W).astype(F32)
    by_row = ((lane // 32) % 2 == 0)[None, :]
    angles = jnp.where(by_row, row_pos[:, None], col_pos[:, None]) * inverse
    sine = jnp.sin(angles)
    return jnp.cos(angles), jnp.where(((lane // 16) % 2 == 0)[None, :], -sine, sine)


def attend(q, key_t, values, mask, sink):
    lane = lax.broadcasted_iota(jnp.int32, (BLK, 128), 1)
    row = lax.broadcasted_iota(jnp.int32, (2 * BLK, 1), 0)
    none = jnp.zeros((BLK, 128), BF16)
    outs = []
    for p in range(GROUP // 2):
        pair = q[:, p * 128 : (p + 1) * 128]
        both = jnp.concatenate(
            [jnp.where(lane < 64, pair, none), jnp.where(lane < 64, none, pair)], axis=0
        )
        scores = dot(both, key_t) + mask
        sinks = jnp.where(row < BLK, sink[2 * p], sink[2 * p + 1])
        highest = jnp.maximum(jnp.max(scores, axis=-1, keepdims=True), sinks)
        expo = jnp.exp(scores - highest)
        denominator = jnp.sum(expo, axis=-1, keepdims=True) + jnp.exp(sinks - highest)
        weights = (expo * (1.0 / denominator)).astype(BF16)
        out = dot(weights, values)
        outs.append(jnp.where(lane < 64, out[:BLK], out[BLK:]).astype(BF16))
    return jnp.concatenate(outs, axis=1)


def twice_keys(kv):
    turned = kv.astype(F32).T
    return jnp.concatenate([turned[:64], turned[:64]], axis=0).astype(BF16)


def twice_values(kv):
    wide = kv.astype(F32)
    lane = lax.broadcasted_iota(jnp.int32, wide.shape, 1)
    return jnp.where(lane < 64, pltpu.roll(wide, 64, 1), wide).astype(BF16)


def band():
    shape = (2 * BLK, 3 * BLK)
    i = lax.broadcasted_iota(jnp.int32, shape, 0) % BLK
    j = lax.broadcasted_iota(jnp.int32, shape, 1)
    return jnp.where((j >= i) & (j <= i + 2 * WINDOW), 0.0, masked_score)


def inner_kernel(sink, query, kv, act, key_t, values, mask):
    mask[...] = band()
    for k in range(ROWS // BLK):
        at = slice(k * BLK, (k + 1) * BLK)
        key_t[:, at] = twice_keys(kv[at, :])
        values[at, :] = twice_values(kv[at, :])

    def block(b, carry):
        start = pl.multiple_of(b * BLK, BLK)
        before = pl.multiple_of(start - BLK, BLK)
        act[pl.ds(start, BLK), 256:] = attend(
            query[pl.ds(start, BLK), :],
            key_t[:, pl.ds(before, 3 * BLK)],
            values[pl.ds(before, 3 * BLK), :],
            mask[...],
            sink,
        )
        return carry

    lax.fori_loop(1, ROWS // BLK - 1, block, 0)


def inner_mixer(sink, query, kv):
    return pl.pallas_call(
        inner_kernel,
        in_specs=[smem(), vmem(), vmem()],
        out_specs=vmem(),
        out_shape=jax.ShapeDtypeStruct((ROWS, 512), BF16),
        scratch_shapes=[
            pltpu.VMEM((128, ROWS), BF16),
            pltpu.VMEM((ROWS, 128), BF16),
            pltpu.VMEM((2 * BLK, 3 * BLK), F32),
        ],
        compiler_params=PARAMS,
        name="inner_mixer",
    )(sink, query, kv)


def rim_kernel(place, sink, query, kv, pool, low, high, weight, scale, inner, act, poolx, ends):
    offset, tp = place[4], place[5]
    act[BLK : ROWS - BLK, 256:] = inner[BLK : ROWS - BLK, 256:]
    last = ROWS - BLK
    lane = lax.broadcasted_iota(jnp.int32, (1, 3 * BLK), 1)
    span = 3 * BLK
    ends[: BLK] = high[:BLK]
    ends[BLK:span] = kv[: 2 * BLK]
    ends[span : span + 2 * BLK] = kv[last - BLK :]
    ends[span + 2 * BLK :] = low[:BLK]

    def end(e, carry):
        start = pl.multiple_of(e * last, BLK)
        keys = ends[pl.ds(pl.multiple_of(e * span, BLK), span), :]
        key_pos = offset + start - WINDOW + lane
        edge = jnp.where((key_pos >= 0) & (key_pos < TOTAL), 0.0, masked_score)
        act[pl.ds(start, BLK), 256:] = attend(
            query[pl.ds(start, BLK), :],
            twice_keys(keys),
            twice_values(keys),
            band() + edge,
            sink,
        )
        return carry

    lax.fori_loop(0, 2, end, 0)

    poolx[:8, :128] = high[136:144].astype(F32)
    poolx[:8, 128:] = high[152:160].astype(F32)
    poolx[8 : 8 + ROWS] = pool[...].astype(F32)
    poolx[8 + ROWS :, :128] = low[128:136].astype(F32)
    poolx[8 + ROWS :, 128:] = low[144:152].astype(F32)
    level = lax.rem(tp, 4)
    half_width = lax.shift_left(jnp.int32(1), level)

    def block(b, carry):
        start = pl.multiple_of(b * BLK, BLK)
        x = poolx[pl.ds(start, BLK + 2 * REACH), :]
        n = BLK + 2 * REACH
        a1 = x + pltpu.roll(x, n - 1, 0)
        a2 = a1 + pltpu.roll(a1, n - 2, 0)
        a3 = a2 + pltpu.roll(a2, n - 4, 0)
        a4 = a3 + pltpu.roll(a3, n - 8, 0)
        window_sum = jnp.where(
            level == 0,
            a1[7 : 7 + BLK],
            jnp.where(
                level == 1, a2[6 : 6 + BLK], jnp.where(level == 2, a3[4 : 4 + BLK], a4[:BLK])
            ),
        )
        t = offset + start + lax.broadcasted_iota(jnp.int32, (BLK, 1), 0)
        counts = jnp.minimum(t + half_width, TOTAL) - jnp.maximum(t - half_width, 0)
        pooled = (window_sum / counts.astype(F32) - x[8 : 8 + BLK]).astype(BF16)
        mixing = dot(pooled, weight[...])
        act[pl.ds(start, BLK), :256] = (mixing * scale[...]).astype(BF16)
        return carry

    lax.fori_loop(0, ROWS // BLK, block, 0)


def rim_mixer(place, sink, query, kv, pool, low, high, weight, scale, inner):
    return pl.pallas_call(
        rim_kernel,
        in_specs=[smem(), smem()] + [vmem()] * 8,
        out_specs=vmem(),
        out_shape=jax.ShapeDtypeStruct((ROWS, 512), BF16),
        scratch_shapes=[
            pltpu.VMEM((ROWS + 2 * REACH, POOL_W), F32),
            pltpu.VMEM((6 * BLK, KV_W), BF16),
        ],
        compiler_params=PARAMS,
        name="rim_mixer",
    )(place, sink, query, kv, pool, low, high, weight, scale.reshape(1, POOL_W), inner)


def out_kernel(steps, place, act, *refs):
    pieces, (keep, send) = refs[:NZ], refs[NZ:]
    z, y, x, c = place[0], place[1], place[2], place[3]
    blocks = []
    for core in (c, 1 - c):
        for step in steps:
            chip = lax.rem(x + step, NX)
            blocks.append(act[pl.ds(pl.multiple_of((chip * 2 + core) * BLK, BLK), BLK), :])
    rows = jnp.concatenate(blocks, axis=0)
    n = len(steps) * BLK
    for q in range(NZ):
        o = dot(rows, pieces[q][...]).astype(BF16)
        zz = lax.rem(z - jnp.where(c == 0, q, -q) + NZ, NZ)
        for t, k in enumerate((0, 2, 1, 3)):
            yy = lax.rem(y - jnp.where(c == 0, k, -k) + NY, NY)
            at = pl.ds(pl.multiple_of((zz * NY + yy) * BLK, BLK), BLK)
            keep[:, at] = o[:n, t * BLK : (t + 1) * BLK]
            send[:, at] = o[n:, t * BLK : (t + 1) * BLK]


def out_chunk(steps, place, act, pieces):
    shape = jax.ShapeDtypeStruct((len(steps) * BLK, D), BF16)
    return pl.pallas_call(
        functools.partial(out_kernel, steps),
        in_specs=[smem()] + [vmem()] * (1 + NZ),
        out_specs=[vmem()] * 2,
        out_shape=[shape] * 2,
        compiler_params=PARAMS,
    )(place, act, *pieces)


def total(*parts):
    return sum(p.astype(F32) for p in parts)


def added(*parts):
    return total(*parts).astype(BF16)


def shards(
    tokens,
    norm_gain,
    pool_in_weight,
    query_weight,
    key_weight,
    value_weight,
    pool_weight,
    pool_scale,
    sink_logit,
    out_pool_weight,
    out_attn_weight,
):
    z, y, x, c = (lax.axis_index(a) for a in ("z", "y", "x", "c"))
    offset = (z * NY + y) * ROWS
    place = jnp.stack([z, y, x, c, offset, x * NC + c]).astype(jnp.int32)

    swap = lambda a: shift(a, "c", NC, 1)

    flat = []
    for t in both_ways(tokens, "x", NX):
        flat += [t, swap(t)]

    w_in = input_block(pool_in_weight, query_weight, key_weight, value_weight)
    quarter = packed(both_ways(w_in, "z", NZ))
    w = both_ways(quarter, "y", NY)

    unit = stacked(out_pool_weight, out_attn_weight)
    unit = joined(unit, shift(unit, "y", NY, 2))
    unit = joined(unit, one_way(unit, "y", 1))
    pieces = both_ways(unit, "z", NZ)

    cos, sin = rotary_rows(offset)
    normed = normed_rows(place, flat, norm_gain)
    acc = first_projection(normed, w[0], w[1], w[3])
    pool, query, kv, low, high = second_projection(normed, w[2], acc, cos, sin)

    count = NZ * NY
    forward = [(i, i + 1) for i in range(count - 1)]
    backward = [(i + 1, i) for i in range(count - 1)]
    from_before = lax.ppermute(high, ("z", "y"), forward)
    from_after = lax.ppermute(low, ("z", "y"), backward)
    inner = inner_mixer(sink_logit, query, kv)
    act = rim_mixer(
        place,
        sink_logit,
        query,
        kv,
        pool,
        from_after,
        from_before,
        pool_weight[0],
        pool_scale,
        inner,
    )

    half = D // 2
    keep2, send2 = out_chunk((2,), place, act, pieces)
    part2 = swap(send2)
    a = shift(added(keep2[:, :half], part2[:, :half]), "x", NX, 1)
    b = shift(added(keep2[:, half:], part2[:, half:]), "x", NX, -1)
    keeps, sends = out_chunk((1, 3), place, act, pieces)
    parts = swap(sends)
    early = lax.optimization_barrier((keeps, parts))
    right_high = shift(added(*[v[:BLK, half:] for v in early]), "x", NX, 1)
    early = lax.optimization_barrier((keeps, parts))
    left_low = shift(added(*[v[BLK:, :half] for v in early]), "x", NX, -1)
    right_low = shift(added(keeps[:BLK, :half], parts[:BLK, :half], a), "x", NX, 1)
    left_high = shift(added(keeps[BLK:, half:], parts[BLK:, half:], b), "x", NX, -1)
    keep0, send0 = out_chunk((0,), place, act, pieces)
    part0 = swap(send0)
    low = total(keep0[:, :half], part0[:, :half], left_low)
    high = total(keep0[:, half:], part0[:, half:], right_high)
    low, high = lax.optimization_barrier((low, high))
    return jnp.concatenate([added(low, right_low), added(high, left_high)], axis=1)


def solution(mesh):
    finer = Mesh(mesh.devices.reshape(NZ, NY, NX, NC), ("z", "y", "x", "c"))
    sp, tp = ("z", "y"), ("x", "c")
    return jax.shard_map(
        shards,
        mesh=finer,
        in_specs=(
            P(sp, tp),
            P(),
            P(sp, tp),
            P(sp, tp),
            P(sp, tp),
            P(sp, tp),
            P(tp, None, None),
            P(tp),
            P(tp),
            P(tp, sp),
            P(tp, sp),
        ),
        out_specs=P(sp + tp, None),
        check_vma=False,
    )
```
